512 devices in a mesh: fs: 128 (over z, y, core), tp: 4 (over x).
Axes of the slice: x: 4, y: 8, z: 8, core: 2. Of those that a mesh axis runs over, the one named last changes fastest.
Arguments:
- tokens: bfloat16 [8192, 2048], P('fs', 'tp'), may hold values from -6 to 6
- norm_gain: float32 [2048], P('fs'), may hold values from 0.1 to 1.9
- gate_weight: float32 [128, 2048, 512], P(None, 'fs', 'tp'), may hold values from -0.125 to 0.125
- up_weight: float32 [128, 2048, 512], P(None, 'fs', 'tp'), may hold values from -0.125 to 0.125
- down_weight: float32 [128, 2048, 512], P(None, 'fs', 'tp'), may hold values from -0.25 to 0.25
- route_ids: int32 [8192, 2], P('fs'), may hold values from 0 to 127, all different within a row; in each aligned block of 64 rows (0 to 63, 64 to 127, ...) at most 2 rows name the same one
- group_weight: float32 [8192], P('fs'), may hold values from 0.3 to 1
- logit_gap: float32 [8192], P('fs'), may hold values from -6 to 6
Outputs:
- gate_new: bfloat16 [128, 2048, 512], P('fs', None, 'tp')
- up_new: bfloat16 [128, 2048, 512], P('fs', None, 'tp')
- down_new: bfloat16 [128, 2048, 512], P('fs', None, 'tp')
- mixed: bfloat16 [8192, 2048], P('fs', 'tp')
The draws below stay inside these ranges and needn't reach their ends.
Inputs may be any that keep to these rules, and one draw needn't show every extreme that they name: `route_ids`: each row names two different experts. In the rows of one device no expert is named by more than 2 rows, a bound that some block reaches.
All inputs are finite; a program needn't handle non-finite values.
Results may differ from the reference program's by a relative error of at most 0.011.
Values may be sent and summed in bfloat16 or wider, within the bound.
A program may use at most 64 MiB of HBM per device.

```python
import math
import jax
import jax.numpy as jnp
import numpy as np
from jax import lax

D = 2048
FF = 512
TOK_DEV = 64
EXPERTS = 128
CAP = 2
TOKENS = 8192
N_FS = 128
N_TP = 4


def block_scale(stream_key, shape, cuts, low, high):
    factor_of = 1.0
    for axis_at, parts in cuts:
        heights = jax.random.uniform(jax.random.fold_in(jax.random.fold_in(stream_key, 6), axis_at), (parts,), jnp.float32, low / len(cuts), high / len(cuts))
        factor_of = factor_of * jnp.repeat(jnp.exp(heights), shape[axis_at] // parts).reshape((-1,) + (1,) * (len(shape) - 1 - axis_at))
    return factor_of


def routed_block(rng, own, number, rows, amount, top, most, slope):
    order = jax.random.permutation(rng, amount)
    heavy_load, ordinary = load_shares(amount, rows * top, most, slope, True), load_shares(amount, rows * top, most, slope, False)
    places = jnp.arange(amount)

    def named(tallies, offset_by):
        used = int((tallies > 0).sum())
        fixed = max(1, used // 4)
        passed = fixed + (places - fixed + offset_by * (used - fixed)) % max(1, amount - fixed)
        return jnp.zeros((amount,), jnp.int32).at[order[jnp.where(places < fixed, places, passed)]].set(jnp.asarray(tallies, jnp.int32))

    tallies = jnp.where(number % 4 == 0, named(heavy_load, number // 4), named(ordinary, number - number // 4 - 1))
    mixed = jax.random.permutation(jax.random.fold_in(own, 3), amount)
    source_of, receiver = mixed[0:amount // 2 * 2:2], mixed[1:amount // 2 * 2:2]
    slack = jnp.minimum(tallies[source_of] - 1, most - tallies[receiver]) // 2
    slack = jnp.where((source_of == order[0]) | (receiver == order[0]) | (tallies[receiver] == 0), 0, jnp.maximum(slack, 0))
    passed = jax.random.randint(jax.random.fold_in(own, 4), (amount // 2,), 0, 1 << 20) % (slack + 1)
    tallies = tallies.at[source_of].add(-passed).at[receiver].add(passed)
    items = jnp.searchsorted(jnp.cumsum(tallies), jnp.arange(rows * top), side="right").astype(jnp.int32)
    table = items.reshape(top, rows).T
    table = table[jax.random.permutation(jax.random.fold_in(own, 1), rows)]
    offset_by = jax.random.randint(jax.random.fold_in(own, 2), (rows, 1), 0, top)
    return jnp.take_along_axis(table, (jnp.arange(top)[None, :] + offset_by) % top, axis=1)


def load_shares(number_of, total, reach, lean, full):
    portions = [(1 << 20) // math.isqrt(grade ** lean) + 1 for grade in range(1, number_of + 1)]
    largest = reach if full else min(reach, max(-(-total // number_of), total * portions[0] // sum(portions)))
    least = 1 if total - largest >= number_of - 1 else 0
    counts, spare = [largest] + [least] * (number_of - 1), total - largest - least * (number_of - 1)
    while spare > 0:
        movable = [i for i in range(1, number_of) if counts[i] < largest] or [i for i in range(1, number_of) if counts[i] < reach]
        pool, budget = sum([portions[i] for i in movable]), spare
        for i in movable:
            extra = min(reach - counts[i], max(1, budget * portions[i] // pool), spare)
            counts[i] = counts[i] + extra
            spare = spare - extra
    return np.array(counts)


def centred(rng, dims, width, most, cuts=(), kind=jnp.bfloat16):
    drawn = jax.random.normal(rng, dims, jnp.float32) * width
    if len(cuts) > 0:
        drawn = block_scale(rng, dims, cuts, -0.22, 0.18) * drawn
    return jnp.clip(drawn, min=-most, max=most).astype(kind)


def setup_inputs(seed: int = 0) -> dict:
    arg_keys = jax.random.split(jax.random.key(seed), 9)
    tokens = centred(arg_keys[0], (TOKENS, D), 1.0, 6.0, ((0, 128), (1, 4)))
    norm_gain = jnp.clip(1.0 + 0.18 * jax.random.normal(arg_keys[1], (D,), jnp.float32), 0.1, 1.9)
    gate_weight = centred(arg_keys[2], (EXPERTS, D, FF), D ** -0.5, 0.125, ((1, 128), (2, 4)), jnp.float32)
    up_weight = centred(arg_keys[3], (EXPERTS, D, FF), D ** -0.5, 0.125, ((1, 128), (2, 4)), jnp.float32)
    down_weight = centred(arg_keys[4], (EXPERTS, D, FF), FF ** -0.5, 0.25, ((1, 128), (2, 4)), jnp.float32)
    route_ids_keys = jax.random.split(jax.random.fold_in(arg_keys[5], 1), TOKENS // TOK_DEV)
    route_ids_turns = jax.random.permutation(jax.random.fold_in(arg_keys[5], 3), TOKENS // TOK_DEV)
    route_ids = jax.vmap(lambda own, number: routed_block(jax.random.fold_in(arg_keys[5], 2), own, number, TOK_DEV, EXPERTS, 2, CAP, 2))(route_ids_keys, route_ids_turns).reshape((TOKENS, 2))
    group_weight = jnp.clip(0.3 + 0.7 * jax.random.uniform(arg_keys[6], (TOKENS,), jnp.float32) ** block_scale(arg_keys[6], (TOKENS,), ((0, 128),), -0.2, 0.2), 0.3, 1.0)
    logit_gap = centred(arg_keys[7], (TOKENS,), 1.5, 6.0, ((0, 128),), jnp.float32)
    return dict(tokens=tokens, norm_gain=norm_gain, gate_weight=gate_weight, up_weight=up_weight, down_weight=down_weight, route_ids=route_ids, group_weight=group_weight, logit_gap=logit_gap)


def reference(tokens, norm_gain, gate_weight, up_weight, down_weight, route_ids, group_weight, logit_gap):
    scaled = norm_gain.astype(jnp.float32)[None, :, None]
    gate_new = (gate_weight * scaled).astype(jnp.bfloat16)
    up_new = (up_weight * scaled).astype(jnp.bfloat16)
    down_new = down_weight.astype(jnp.bfloat16)
    pair_count = 2 * TOK_DEV
    flat_ids = route_ids.reshape(N_FS, pair_count).astype(jnp.int32)
    onehot = (flat_ids[:, :, None] == jnp.arange(EXPERTS, dtype=jnp.int32)[None, None, :]).astype(jnp.float32)
    before = jnp.cumsum(onehot, axis=1) - onehot
    ranked = jnp.sum(before * onehot, axis=2).astype(jnp.int32)
    slot_ids = flat_ids * CAP + ranked
    owners = jnp.broadcast_to((jnp.arange(pair_count, dtype=jnp.int32) // 2)[None, :], (N_FS, pair_count))
    blocks = jnp.broadcast_to(jnp.arange(N_FS, dtype=jnp.int32)[:, None], (N_FS, pair_count))
    slot_table = jnp.full((N_FS, EXPERTS * CAP), TOK_DEV, jnp.int32).at[blocks, slot_ids].set(owners)
    padded = jnp.concatenate([tokens.reshape(N_FS, TOK_DEV, D), jnp.zeros((N_FS, 1, D), jnp.bfloat16)], axis=1)
    source_ids = jnp.arange(N_FS, dtype=jnp.int32)[:, None]

    def one_expert(expert):
        picked = lax.dynamic_slice_in_dim(slot_table, expert * CAP, CAP, 1)
        slot_rows = padded[source_ids, picked].reshape(N_FS * CAP, D)
        gate_acc = jnp.dot(slot_rows, gate_new[expert], preferred_element_type=jnp.float32)
        up_acc = jnp.dot(slot_rows, up_new[expert], preferred_element_type=jnp.float32)
        hidden = (jax.nn.silu(gate_acc) * up_acc).astype(jnp.bfloat16)
        pieces = hidden.reshape(N_FS * CAP, N_TP, FF // N_TP).astype(jnp.float32)
        down_pieces = down_new[expert].reshape(D, N_TP, FF // N_TP).astype(jnp.float32)
        partial_value = jnp.einsum('rjf,djf->jrd', pieces, down_pieces).astype(jnp.bfloat16)
        partial_value = lax.optimization_barrier(partial_value)
        summed = jnp.sum(partial_value.astype(jnp.float32), axis=0).astype(jnp.bfloat16)
        return summed.reshape(N_FS, CAP, D)

    outputs = lax.map(one_expert, jnp.arange(EXPERTS, dtype=jnp.int32))
    gathered = outputs[flat_ids, blocks, ranked].reshape(TOKENS, 2, D).astype(jnp.float32)
    gap = logit_gap.astype(jnp.float32)
    first_weight = group_weight * jax.nn.sigmoid(gap)
    second_weight = group_weight * jax.nn.sigmoid(-gap)
    mixed = (first_weight[:, None] * gathered[:, 0] + second_weight[:, None] * gathered[:, 1]).astype(jnp.bfloat16)
    return gate_new, up_new, down_new, mixed
```

```python
import functools

import jax
import jax.numpy as jnp
from jax import lax
from jax.experimental import pallas as pl
from jax.experimental.pallas import tpu as pltpu
from jax.sharding import PartitionSpec as P

MESH = pl.DeviceIdType.MESH
F32, BF16 = jnp.float32, jnp.bfloat16
STRIDE = 45


def partner(me, off):
    z, y, c = me // 16, (me // 2) % 8, me % 2
    dz, dy, dc = off // 16, (off // 2) % 8, off % 2
    return ((z + dz) % 8) * 16 + ((y + dy) % 8) * 2 + (c + dc) % 2


def each_partner(me, n_fs, step):
    def turn(i, off):
        step(partner(me, off))
        later = off + STRIDE
        return jnp.where(later >= n_fs, later - (n_fs - 1), later)

    lax.fori_loop(0, n_fs - 1, turn, jnp.int32(1))


def kernel(
    n_fs, n_tp,
    ids_ref, group_ref, gap_ref, gain_ref, tokens_ref, gate_ref, up_ref, down_ref,
    gate_in, up_in, down_in, mixed_ref,
    ids, group, gap, gain, tokens, gate_f, up_f, down_f,
    gate_out, up_out, down_out, tok_out, tok_in, ret_out, ret_in,
    rows_all, hid_all, down_q, wide, picks,
    local_sem, send_sem, recv_sem,
):
    me, j = lax.axis_index("fs"), lax.axis_index("tp")
    slots = 2 * n_fs
    barrier = pltpu.get_barrier_semaphore()

    def greet(d):
        pl.semaphore_signal(barrier, inc=1, device_id={"fs": d}, device_id_type=MESH)

    each_partner(me, n_fs, greet)
    for k in range(1, n_tp):
        pl.semaphore_signal(
            barrier, inc=1, device_id={"tp": (j + k) % n_tp}, device_id_type=MESH
        )

    small = [(ids_ref, ids), (group_ref, group), (gap_ref, gap), (gain_ref, gain), (tokens_ref, tokens)]
    large = [(down_ref, down_f), (gate_ref, gate_f), (up_ref, up_f)]
    loads = [
        pltpu.make_async_copy(src, dst, local_sem.at[i])
        for i, (src, dst) in enumerate(small + large)
    ]
    for c in loads:
        c.start()
    for c in loads[:5]:
        c.wait()

    count = tokens.shape[0]
    slot = lax.broadcasted_iota(jnp.int32, (slots, count), 0)
    first = (slot // 2 == ids[0:1, :]).astype(F32)
    second = (slot // 2 == ids[1:2, :]).astype(F32)
    earlier = (
        lax.broadcasted_iota(jnp.int32, (count, count), 0)
        < lax.broadcasted_iota(jnp.int32, (count, count), 1)
    ).astype(BF16)
    before = jnp.dot((first + second).astype(BF16), earlier, preferred_element_type=F32)
    ranked = (before == (slot % 2).astype(F32)).astype(F32)
    first, second = first * ranked, second * ranked
    picks[0] = first.astype(BF16)
    picks[1] = second.astype(BF16)
    outgoing = jnp.dot((first + second).astype(BF16), tokens[...], preferred_element_type=F32)
    for b in range(4):
        wide[pl.ds(b, slots, stride=4), :] = outgoing[:, b * 128 : (b + 1) * 128]
    tok_out[...] = wide[...].astype(BF16).reshape(n_fs, 8, 128)

    diagonal = lax.broadcasted_iota(jnp.int32, (16, 16), 0) == lax.broadcasted_iota(
        jnp.int32, (16, 16), 1
    )
    scale = jnp.sum(jnp.where(diagonal, gain[...], 0.0), axis=1, keepdims=True)
    scale = jnp.broadcast_to(scale, (16, 128))[None]

    def round_down(i, _):
        at = pl.ds(i * 8, 8)
        down_out[at] = down_f[at].astype(BF16)
        return 0

    def round_first(i, _):
        at = pl.ds(i * 8, 8)
        gate_out[at] = (gate_f[at] * scale).astype(BF16)
        up_out[at] = (up_f[at] * scale).astype(BF16)
        return 0

    loads[5].wait()
    lax.fori_loop(0, n_fs // 8, round_down, 0)
    loads[6].wait()
    loads[7].wait()
    lax.fori_loop(0, n_fs // 8, round_first, 0)

    pl.semaphore_wait(barrier, n_fs - 1 + n_tp - 1)

    def exchange(i, src, dst):
        def send(d):
            pltpu.make_async_remote_copy(
                src_ref=src.at[d], dst_ref=dst.at[me],
                send_sem=send_sem.at[i], recv_sem=recv_sem.at[i],
                device_id={"fs": d}, device_id_type=MESH,
            ).start()

        each_partner(me, n_fs, send)
        dst[me] = src[me]

    def all_of(i, src, dst, copies=n_fs - 1):
        return pltpu.make_async_remote_copy(
            src_ref=src.at[pl.ds(0, copies)], dst_ref=dst.at[pl.ds(0, copies)],
            send_sem=send_sem.at[i], recv_sem=recv_sem.at[i],
            device_id={"tp": (j + 1) % n_tp}, device_id_type=MESH,
        )

    exchange(0, tok_out, tok_in)
    exchange(1, down_out, down_in)
    exchange(2, gate_out, gate_in)
    exchange(3, up_out, up_in)

    def across(i, src_of, dst):
        for k in range(1, n_tp):
            to = (j + k) % n_tp
            pltpu.make_async_remote_copy(
                src_ref=src_of(to), dst_ref=dst.at[j],
                send_sem=send_sem.at[i], recv_sem=recv_sem.at[i],
                device_id={"tp": to}, device_id_type=MESH,
            ).start()

    all_of(0, tok_out, tok_in).wait_recv()
    wide[...] = tok_in[...].reshape(slots * 4, 128).astype(F32)
    for b in range(4):
        rows_all[j, :, b * 128 : (b + 1) * 128] = wide[pl.ds(b, slots, stride=4), :].astype(BF16)
    across(4, lambda to: rows_all.at[j], rows_all)

    all_of(1, down_out, down_in).wait_recv()
    across(5, lambda to: down_in.at[pl.ds(to * (n_fs // n_tp), n_fs // n_tp)], down_q)
    down_q[j] = down_in[pl.ds(j * (n_fs // n_tp), n_fs // n_tp)]

    all_of(4, rows_all, rows_all, n_tp - 1).wait_recv()
    all_of(2, gate_out, gate_in).wait_recv()
    depth = n_fs // n_tp

    def product(w):
        total = None
        for k in range(n_tp):
            block = w[k * depth : (k + 1) * depth].reshape(depth * 16, 128)
            term = jnp.dot(rows_all[k], block, preferred_element_type=F32)
            total = term if total is None else total + term
        return total

    gate_acc = product(gate_in)
    all_of(3, up_out, up_in).wait_recv()
    up_acc = product(up_in)
    hid_all[j] = (gate_acc / (1.0 + jnp.exp(-gate_acc)) * up_acc).astype(BF16)
    across(6, lambda to: hid_all.at[j], hid_all)
    all_of(5, down_q, down_q, n_tp - 1).wait_recv()
    all_of(6, hid_all, hid_all, n_tp - 1).wait_recv()
    total = None
    for k in range(n_tp):
        term = lax.dot_general(
            hid_all[k], down_q[k].reshape(depth * 16, 128), (((1,), (1,)), ((), ())),
            preferred_element_type=F32,
        )
        total = term if total is None else total + term
    for b in range(4):
        wide[pl.ds(b, slots, stride=4), :] = total[:, b * 128 : (b + 1) * 128]
    ret_out[...] = wide[...].astype(BF16).reshape(n_fs, 8, 128)
    exchange(7, ret_out, ret_in)

    here = lax.broadcasted_iota(jnp.int32, (count, count), 0) == lax.broadcasted_iota(
        jnp.int32, (count, count), 1
    )
    w_first = group[...] * jax.nn.sigmoid(gap[...])
    w_second = group[...] * jax.nn.sigmoid(-gap[...])
    w_first = jnp.sum(jnp.where(here, w_first, 0.0), axis=1, keepdims=True)
    w_second = jnp.sum(jnp.where(here, w_second, 0.0), axis=1, keepdims=True)

    all_of(7, ret_out, ret_in).wait_recv()
    wide[...] = ret_in[...].reshape(slots * 4, 128).astype(F32)
    for b in range(4):
        block = wide[pl.ds(b, slots, stride=4), :].astype(BF16)
        value = [
            lax.dot_general(
                picks[k], block, (((0,), (0,)), ((), ())), preferred_element_type=F32
            )
            for k in range(2)
        ]
        mixed_ref[:, b * 128 : (b + 1) * 128] = (
            w_first * value[0] + w_second * value[1]
        ).astype(BF16)

    for i, (src, dst) in enumerate(
        [(tok_out, tok_in), (down_out, down_in), (gate_out, gate_in), (up_out, up_in)]
    ):
        all_of(i, src, dst).wait_send()
    for i, a in ((4, rows_all), (5, down_q), (6, hid_all)):
        all_of(i, a, a, n_tp - 1).wait_send()
    all_of(7, ret_out, ret_in).wait_send()


def body(
    tokens, norm_gain, gate_weight, up_weight, down_weight, route_ids, group_weight, logit_gap
):
    n_fs, n_tp = lax.axis_size("fs"), lax.axis_size("tp")
    count, width = tokens.shape
    experts, depth, units = gate_weight.shape
    whole = pl.BlockSpec(memory_space=pltpu.VMEM)
    anywhere = pl.BlockSpec(memory_space=pl.ANY)
    weights = jax.ShapeDtypeStruct((experts, depth, units), BF16)
    slots = 2 * n_fs
    gate_new, up_new, down_new, mixed = pl.pallas_call(
        functools.partial(kernel, n_fs, n_tp),
        out_shape=(weights, weights, weights, jax.ShapeDtypeStruct((count, width), BF16)),
        in_specs=[anywhere] * 8,
        out_specs=[whole] * 4,
        scratch_shapes=[
            pltpu.VMEM((2, count), jnp.int32),
            pltpu.VMEM((1, count), F32),
            pltpu.VMEM((1, count), F32),
            pltpu.VMEM((1, depth), F32),
            pltpu.VMEM((count, width), BF16),
        ]
        + [pltpu.VMEM((experts, depth, units), F32)] * 3
        + [pltpu.VMEM((experts, depth, units), BF16)] * 3
        + [pltpu.VMEM((n_fs, 8, 128), BF16)] * 4
        + [
            pltpu.VMEM((n_tp, slots, width), BF16),
            pltpu.VMEM((n_tp, slots, units), BF16),
            pltpu.VMEM((n_tp, n_fs // n_tp, depth, units), BF16),
            pltpu.VMEM((slots * 4, 128), F32),
            pltpu.VMEM((2, slots, count), BF16),
            pltpu.SemaphoreType.DMA((8,)),
            pltpu.SemaphoreType.DMA((8,)),
            pltpu.SemaphoreType.DMA((8,)),
        ],
        compiler_params=pltpu.CompilerParams(
            collective_id=0, has_side_effects=True, vmem_limit_bytes=40 * 1024 * 1024
        ),
    )(
        route_ids.T, group_weight.reshape(1, count), logit_gap.reshape(1, count),
        norm_gain.reshape(1, depth), tokens, gate_weight, up_weight, down_weight,
    )
    shape = (1, experts * depth, units)
    return gate_new.reshape(shape), up_new.reshape(shape), down_new.reshape(shape), mixed


def solution(mesh):
    return jax.shard_map(
        body,
        mesh=mesh,
        in_specs=(
            P("fs", "tp"), P("fs"), P(None, "fs", "tp"), P(None, "fs", "tp"),
            P(None, "fs", "tp"), P("fs", None), P("fs"), P("fs"),
        ),
        out_specs=(P("fs", None, "tp"), P("fs", None, "tp"), P("fs", None, "tp"), P("fs", "tp")),
        check_vma=False,
    )
```

```python
import functools

import jax
import jax.numpy as jnp
from jax import lax
from jax.experimental import pallas as pl
from jax.experimental.pallas import tpu as pltpu
from jax.sharding import PartitionSpec as P

MESH = pl.DeviceIdType.MESH
F32, BF16 = jnp.float32, jnp.bfloat16
STRIDE = 45
FAR_FIRST = (4, 3, 5, 2, 6, 1, 7, 0)


def partner(me, dz, dy, dc):
    z, y, c = me // 16, (me // 2) % 8, me % 2
    return ((z + dz) % 8) * 16 + ((y + dy) % 8) * 2 + (c + dc) % 2


def each_partner(me, n_fs, step):
    def at(n):
        off = (n * STRIDE) % n_fs
        step(partner(me, off // 16, (off // 2) % 8, off % 2))

    def turn(i, _):
        for u in range(8):
            at(i * 8 + u)
        return 0

    for u in range(1, 8):
        at(u)
    lax.fori_loop(1, n_fs // 8, turn, 0)


def far_partners_first(me, step):
    def turn(k, _):
        dz = (4 + (1 - 2 * (k % 2)) * ((k + 1) // 2)) % 8
        for dy in FAR_FIRST:
            for dc in range(2):
                step(partner(me, dz, dy, dc))
        return 0

    lax.fori_loop(0, 7, turn, 0)
    for dy in FAR_FIRST:
        for dc in range(2):
            if dy or dc:
                step(partner(me, 0, dy, dc))


def each_partner_of_rows(me, low, high, step):
    z, y, c = me // 16, (me // 2) % 8, me % 2

    def turn(row, _):
        for dy in FAR_FIRST[:-1]:
            for dc in range(2):
                step(row * 16 + ((y + dy) % 8) * 2 + (c + dc) % 2)
        step(row * 16 + y * 2 + (c + 1) % 2)

        @pl.when(row != z)
        def _():
            step(row * 16 + y * 2 + c)

        return 0

    lax.fori_loop(low, high, turn, 0)


def kernel(
    n_fs, n_tp,
    ids_ref, group_ref, gap_ref, gain_ref, tokens_ref, gate_ref, up_ref, down_ref,
    gate_in, up_in, down_in, mixed_ref,
    ids, group, gap, gain, tokens, gate_f, up_f, down_f,
    gate_out, up_out, down_out, tok_out, tok_in, ret_out, ret_in,
    rows_all, hid_all, down_q, wide, picks,
    local_sem, send_sem, recv_sem,
):
    me, j = lax.axis_index("fs"), lax.axis_index("tp")
    slots = 2 * n_fs
    barrier = pltpu.get_barrier_semaphore()

    def greet(d):
        pl.semaphore_signal(barrier, inc=1, device_id={"fs": d}, device_id_type=MESH)

    small = [(ids_ref, ids), (group_ref, group), (gap_ref, gap), (gain_ref, gain), (tokens_ref, tokens)]
    large = [(down_ref, down_f), (gate_ref, gate_f), (up_ref, up_f)]
    loads = [
        pltpu.make_async_copy(src, dst, local_sem.at[i])
        for i, (src, dst) in enumerate(small + large)
    ]
    for c in loads:
        c.start()
    far_partners_first(me, greet)
    for k in range(1, n_tp):
        pl.semaphore_signal(
            barrier, inc=1, device_id={"tp": (j + k) % n_tp}, device_id_type=MESH
        )
    for c in loads[:5]:
        c.wait()

    count = tokens.shape[0]
    slot = lax.broadcasted_iota(jnp.int32, (slots, count), 0)
    first = (slot // 2 == ids[0:1, :]).astype(F32)
    second = (slot // 2 == ids[1:2, :]).astype(F32)
    earlier = (
        lax.broadcasted_iota(jnp.int32, (count, count), 0)
        < lax.broadcasted_iota(jnp.int32, (count, count), 1)
    ).astype(BF16)
    before = jnp.dot((first + second).astype(BF16), earlier, preferred_element_type=F32)
    ranked = (before == (slot % 2).astype(F32)).astype(F32)
    first, second = first * ranked, second * ranked
    picks[0] = first.astype(BF16)
    picks[1] = second.astype(BF16)
    outgoing = jnp.dot((first + second).astype(BF16), tokens[...], preferred_element_type=F32)
    for b in range(4):
        wide[pl.ds(b, slots, stride=4), :] = outgoing[:, b * 128 : (b + 1) * 128]
    tok_out[...] = wide[...].astype(BF16).reshape(n_fs, 8, 128)

    diagonal = lax.broadcasted_iota(jnp.int32, (16, 16), 0) == lax.broadcasted_iota(
        jnp.int32, (16, 16), 1
    )
    scale = jnp.sum(jnp.where(diagonal, gain[...], 0.0), axis=1, keepdims=True)
    scale = jnp.broadcast_to(scale, (16, 128))[None]

    def round_down(i, _):
        at = pl.ds(i * 8, 8)
        down_out[at] = down_f[at].astype(BF16)
        return 0

    def round_first(i, _):
        at = pl.ds(i * 8, 8)
        gate_out[at] = (gate_f[at] * scale).astype(BF16)
        up_out[at] = (up_f[at] * scale).astype(BF16)
        return 0

    pl.semaphore_wait(barrier, n_fs - 1 + n_tp - 1)

    def sender(i, src, dst):
        def send(d):
            pltpu.make_async_remote_copy(
                src_ref=src.at[d], dst_ref=dst.at[me],
                send_sem=send_sem.at[i], recv_sem=recv_sem.at[i],
                device_id={"fs": d}, device_id_type=MESH,
            ).start()

        return send

    def exchange(i, src, dst):
        each_partner(me, n_fs, sender(i, src, dst))
        dst[me] = src[me]

    def all_of(i, src, dst, copies=n_fs - 1):
        return pltpu.make_async_remote_copy(
            src_ref=src.at[pl.ds(0, copies)], dst_ref=dst.at[pl.ds(0, copies)],
            send_sem=send_sem.at[i], recv_sem=recv_sem.at[i],
            device_id={"tp": (j + 1) % n_tp}, device_id_type=MESH,
        )

    exchange(0, tok_out, tok_in)
    loads[5].wait()
    lax.fori_loop(0, n_fs // 8, round_down, 0)
    exchange(1, down_out, down_in)
    loads[6].wait()
    loads[7].wait()
    lax.fori_loop(0, n_fs // 8, round_first, 0)
    exchange(2, gate_out, gate_in)
    exchange(3, up_out, up_in)

    def across(i, src_of, dst):
        for k in (2, 1, 3):
            to = (j + k) % n_tp
            pltpu.make_async_remote_copy(
                src_ref=src_of(to), dst_ref=dst,
                send_sem=send_sem.at[i], recv_sem=recv_sem.at[i],
                device_id={"tp": to}, device_id_type=MESH,
            ).start()

    all_of(0, tok_out, tok_in).wait_recv()
    wide[...] = tok_in[...].reshape(slots * 4, 128).astype(F32)
    for b in range(4):
        rows_all[j, :, b * 128 : (b + 1) * 128] = wide[pl.ds(b, slots, stride=4), :].astype(BF16)
    across(4, lambda to: rows_all.at[j], rows_all.at[j])

    all_of(1, down_out, down_in).wait_recv()
    across(5, lambda to: down_in.at[pl.ds(to * (n_fs // n_tp), n_fs // n_tp)], down_q.at[j])
    down_q[j] = down_in[pl.ds(j * (n_fs // n_tp), n_fs // n_tp)]

    all_of(4, rows_all, rows_all, n_tp - 1).wait_recv()
    all_of(2, gate_out, gate_in).wait_recv()
    depth = n_fs // n_tp

    def product(w):
        total = None
        for k in range(n_tp):
            block = w[k * depth : (k + 1) * depth].reshape(depth * 16, 128)
            term = jnp.dot(rows_all[k], block, preferred_element_type=F32)
            total = term if total is None else total + term
        return total

    gate_acc = product(gate_in)
    all_of(3, up_out, up_in).wait_recv()
    up_acc = product(up_in)
    hidden = (gate_acc / (1.0 + jnp.exp(-gate_acc)) * up_acc).astype(BF16)
    for h in range(2):
        hid_all[h, j] = hidden[h * n_fs : (h + 1) * n_fs]
        across(6 + h, lambda to: hid_all.at[h, j], hid_all.at[h, j])
    all_of(5, down_q, down_q, n_tp - 1).wait_recv()

    for h in range(2):
        all_of(6 + h, hid_all.at[h], hid_all.at[h], n_tp - 1).wait_recv()
        total = None
        for k in range(n_tp):
            term = lax.dot_general(
                hid_all[h, k], down_q[k].reshape(depth * 16, 128), (((1,), (1,)), ((), ())),
                preferred_element_type=F32,
            )
            total = term if total is None else total + term
        for b in range(4):
            wide[pl.ds(h * slots * 2 + b, n_fs, stride=4), :] = total[:, b * 128 : (b + 1) * 128]
        half = pl.ds(h * n_fs // 2, n_fs // 2)
        ret_out[half] = (
            wide[h * slots * 2 : (h + 1) * slots * 2].astype(BF16).reshape(n_fs // 2, 8, 128)
        )
        each_partner_of_rows(me, h * 4, h * 4 + 4, sender(8, ret_out, ret_in))
    ret_in[me] = ret_out[me]

    here = lax.broadcasted_iota(jnp.int32, (count, count), 0) == lax.broadcasted_iota(
        jnp.int32, (count, count), 1
    )
    w_first = group[...] * jax.nn.sigmoid(gap[...])
    w_second = group[...] * jax.nn.sigmoid(-gap[...])
    w_first = jnp.sum(jnp.where(here, w_first, 0.0), axis=1, keepdims=True)
    w_second = jnp.sum(jnp.where(here, w_second, 0.0), axis=1, keepdims=True)

    all_of(8, ret_out, ret_in).wait_recv()
    wide[...] = ret_in[...].reshape(slots * 4, 128).astype(F32)
    for b in range(4):
        block = wide[pl.ds(b, slots, stride=4), :].astype(BF16)
        value = [
            lax.dot_general(
                picks[k], block, (((0,), (0,)), ((), ())), preferred_element_type=F32
            )
            for k in range(2)
        ]
        mixed_ref[:, b * 128 : (b + 1) * 128] = (
            w_first * value[0] + w_second * value[1]
        ).astype(BF16)

    for i, (src, dst) in enumerate(
        [(tok_out, tok_in), (down_out, down_in), (gate_out, gate_in), (up_out, up_in)]
    ):
        all_of(i, src, dst).wait_send()
    for i, a in ((4, rows_all), (5, down_q), (6, hid_all.at[0]), (7, hid_all.at[1])):
        all_of(i, a, a, n_tp - 1).wait_send()
    all_of(8, ret_out, ret_in).wait_send()


def place(gate_in, up_in, down_in, mixed_in, gate_ref, up_ref, down_ref, mixed_ref, sem):
    copies = [
        pltpu.make_async_copy(src, dst, sem.at[i])
        for i, (src, dst) in enumerate(
            [(gate_in, gate_ref), (up_in, up_ref), (down_in, down_ref), (mixed_in, mixed_ref)]
        )
    ]
    for c in copies:
        c.start()
    for c in copies:
        c.wait()


def body(
    tokens, norm_gain, gate_weight, up_weight, down_weight, route_ids, group_weight, logit_gap
):
    n_fs, n_tp = lax.axis_size("fs"), lax.axis_size("tp")
    count, width = tokens.shape
    experts, depth, units = gate_weight.shape
    whole = pl.BlockSpec(memory_space=pltpu.VMEM)
    anywhere = pl.BlockSpec(memory_space=pltpu.HBM)
    weights = jax.ShapeDtypeStruct((experts, depth, units), BF16)
    slots = 2 * n_fs
    results = (weights, weights, weights, jax.ShapeDtypeStruct((count, width), BF16))
    held = pl.pallas_call(
        functools.partial(kernel, n_fs, n_tp),
        out_shape=tuple(pltpu.VMEM(r.shape, r.dtype) for r in results),
        in_specs=[anywhere] * 8,
        out_specs=[whole] * 4,
        scratch_shapes=[
            pltpu.VMEM((2, count), jnp.int32),
            pltpu.VMEM((1, count), F32),
            pltpu.VMEM((1, count), F32),
            pltpu.VMEM((1, depth), F32),
            pltpu.VMEM((count, width), BF16),
        ]
        + [pltpu.VMEM((experts, depth, units), F32)] * 3
        + [pltpu.VMEM((experts, depth, units), BF16)] * 3
        + [pltpu.VMEM((n_fs, 8, 128), BF16)] * 4
        + [
            pltpu.VMEM((n_tp, slots, width), BF16),
            pltpu.VMEM((2, n_tp, n_fs, units), BF16),
            pltpu.VMEM((n_tp, n_fs // n_tp, depth, units), BF16),
            pltpu.VMEM((slots * 4, 128), F32),
            pltpu.VMEM((2, slots, count), BF16),
            pltpu.SemaphoreType.DMA((8,)),
            pltpu.SemaphoreType.DMA((9,)),
            pltpu.SemaphoreType.DMA((9,)),
        ],
        compiler_params=pltpu.CompilerParams(
            collective_id=0, has_side_effects=True, vmem_limit_bytes=65404928 - 8192
        ),
    )(
        route_ids.T, group_weight.reshape(1, count), logit_gap.reshape(1, count),
        norm_gain.reshape(1, depth), tokens, gate_weight, up_weight, down_weight,
    )
    gate_new, up_new, down_new, mixed = pl.pallas_call(
        place,
        out_shape=results,
        in_specs=[whole] * 4,
        out_specs=[anywhere] * 4,
        scratch_shapes=[pltpu.SemaphoreType.DMA((4,))],
        compiler_params=pltpu.CompilerParams(vmem_limit_bytes=4 * 1024 * 1024),
    )(*held)
    shape = (1, experts * depth, units)
    return gate_new.reshape(shape), up_new.reshape(shape), down_new.reshape(shape), mixed


def solution(mesh):
    return jax.shard_map(
        body,
        mesh=mesh,
        in_specs=(
            P("fs", "tp"), P("fs"), P(None, "fs", "tp"), P(None, "fs", "tp"),
            P(None, "fs", "tp"), P("fs", None), P("fs"), P("fs"),
        ),
        out_specs=(P("fs", None, "tp"), P("fs", None, "tp"), P("fs", None, "tp"), P("fs", "tp")),
        check_vma=False,
    )
```

```python
import functools

import jax
import jax.numpy as jnp
from jax import lax
from jax.experimental import pallas as pl
from jax.experimental.pallas import tpu as pltpu
from jax.sharding import PartitionSpec as P

MESH = pl.DeviceIdType.MESH
F32, BF16 = jnp.float32, jnp.bfloat16
FAR_FIRST = (4, 3, 5, 2, 6, 1, 7, 0)
NEARING = sorted(
    ((a, b) for a in range(8) for b in range(8)),
    key=lambda t: -sum(min(FAR_FIRST[i], 8 - FAR_FIRST[i]) for i in t),
)
PIECES = 4


class Torus:
    def __init__(self, me):
        self.z, y, self.c = me // 16, (me // 2) % 8, me % 2
        self.places = [((y + dy) % 8) * 2 for dy in FAR_FIRST]
        self.columns = [at + (self.c + dc) % 2 for at in self.places for dc in (1, 0)]
        self.rows = tuple(((self.z + dz) % 8) * 16 for dz in FAR_FIRST)

    def far_first(self, step):
        def turn(_, rows):
            for column in self.columns:
                step(rows[0] + column)
            return rows[1:] + rows[:1]

        rows = lax.fori_loop(0, 7, turn, self.rows)
        for column in self.columns[:-1]:
            step(rows[0] + column)

    def of_core_far_first(self, core, step):
        for a, b in NEARING:
            if a < 7 or b < 7:
                step(self.rows[a] + self.places[b] + core)

        @pl.when(self.c != core)
        def _():
            step(self.rows[7] + self.places[7] + core)

    def of_core(self, core, step):
        own, columns = self.c == core, [at + core for at in self.places]

        def turn(_, rows):
            for u, column in enumerate(columns):
                step(rows[(3 * u + 2) % 8] + column)
            return rows[1:] + rows[:1]

        for u, column in enumerate(columns[:-1]):
            step(self.rows[(3 * u + 2) % 8] + column)

        @pl.when(jnp.logical_not(own))
        def _():
            step(self.rows[-1] + columns[-1])

        lax.fori_loop(1, 8, turn, self.rows[1:] + self.rows[:1])

    def row_by_row(self, low, high, step):
        def turn(row, _):
            for column in self.columns[:-1]:
                step(row * 16 + column)

            @pl.when(row != self.z)
            def _():
                step(row * 16 + self.columns[-1])

            return 0

        lax.fori_loop(low, high, turn, 0)


def kernel(
    n_fs, n_tp,
    ids_ref, group_ref, gap_ref, gain_ref, tokens_ref, gate_ref, up_ref, down_ref,
    gate_in, up_in, down_in, mixed_ref,
    ids, group, gap, gain, tokens, gate_f, up_f, down_f,
    gate_out, up_out, down_out, tok_out, tok_in, ret_out, ret_in,
    rows_all, hid_all, down_q, wide, picks,
    local_sem, send_sem, recv_sem,
):
    me, j = lax.axis_index("fs"), lax.axis_index("tp")
    slots = 2 * n_fs
    torus = Torus(me)
    barrier = pltpu.get_barrier_semaphore()

    def greet(d):
        pl.semaphore_signal(barrier, inc=1, device_id={"fs": d}, device_id_type=MESH)

    small = [(ids_ref, ids), (group_ref, group), (gap_ref, gap), (gain_ref, gain), (tokens_ref, tokens)]
    large = [(down_ref, down_f), (gate_ref, gate_f), (up_ref, up_f)]
    loads = [
        pltpu.make_async_copy(src, dst, local_sem.at[i])
        for i, (src, dst) in enumerate(small + large)
    ]
    for c in loads:
        c.start()
    torus.far_first(greet)
    for k in range(1, n_tp):
        pl.semaphore_signal(
            barrier, inc=1, device_id={"tp": (j + k) % n_tp}, device_id_type=MESH
        )
    for c in loads[:5]:
        c.wait()

    count = tokens.shape[0]
    slot = lax.broadcasted_iota(jnp.int32, (slots, count), 0)
    first = (slot // 2 == ids[0:1, :]).astype(F32)
    second = (slot // 2 == ids[1:2, :]).astype(F32)
    earlier = (
        lax.broadcasted_iota(jnp.int32, (count, count), 0)
        < lax.broadcasted_iota(jnp.int32, (count, count), 1)
    ).astype(BF16)
    before = jnp.dot((first + second).astype(BF16), earlier, preferred_element_type=F32)
    ranked = (before == (slot % 2).astype(F32)).astype(F32)
    first, second = first * ranked, second * ranked
    picks[0] = first.astype(BF16)
    picks[1] = second.astype(BF16)
    outgoing = jnp.dot((first + second).astype(BF16), tokens[...], preferred_element_type=F32)
    for b in range(4):
        wide[pl.ds(b, slots, stride=4), :] = outgoing[:, b * 128 : (b + 1) * 128]
    tok_out[...] = wide[...].astype(BF16).reshape(n_fs, 8, 128)

    diagonal = lax.broadcasted_iota(jnp.int32, (16, 16), 0) == lax.broadcasted_iota(
        jnp.int32, (16, 16), 1
    )
    scale = jnp.sum(jnp.where(diagonal, gain[...], 0.0), axis=1, keepdims=True)
    scale = jnp.broadcast_to(scale, (16, 128))[None]

    def round_down(i, _):
        at = pl.ds(i * 8, 8)
        down_out[at] = down_f[at].astype(BF16)
        return 0

    def round_first(i, _):
        at = pl.ds(i * 8, 8)
        gate_out[at] = (gate_f[at] * scale).astype(BF16)
        up_out[at] = (up_f[at] * scale).astype(BF16)
        return 0

    pl.semaphore_wait(barrier, n_fs - 1 + n_tp - 1)

    def sender(i, src, dst):
        def send(d):
            pltpu.make_async_remote_copy(
                src_ref=src.at[d], dst_ref=dst.at[me],
                send_sem=send_sem.at[i], recv_sem=recv_sem.at[i],
                device_id={"fs": d}, device_id_type=MESH,
            ).start()

        return send

    def exchange(i, src, dst, core):
        torus.of_core(core, sender(i, src, dst))

    def all_of(i, src, dst, copies=n_fs - 1):
        return pltpu.make_async_remote_copy(
            src_ref=src.at[pl.ds(0, copies)], dst_ref=dst.at[pl.ds(0, copies)],
            send_sem=send_sem.at[i], recv_sem=recv_sem.at[i],
            device_id={"tp": (j + 1) % n_tp}, device_id_type=MESH,
        )

    exchange(0, tok_out, tok_in, 0)
    loads[5].wait()
    lax.fori_loop(0, n_fs // 8, round_down, 0)
    exchange(1, down_out, down_in, 0)
    loads[6].wait()
    loads[7].wait()
    lax.fori_loop(0, n_fs // 8, round_first, 0)
    exchange(2, gate_out, gate_in, 0)
    torus.of_core_far_first(0, sender(3, up_out, up_in))
    exchange(0, tok_out, tok_in, 1)
    exchange(1, down_out, down_in, 1)
    exchange(2, gate_out, gate_in, 1)
    torus.of_core_far_first(1, sender(3, up_out, up_in))
    for src, dst in ((tok_out, tok_in), (down_out, down_in), (gate_out, gate_in), (up_out, up_in)):
        dst[me] = src[me]

    def across(i, src_of, dst):
        for k in (2, 1, 3):
            to = (j + k) % n_tp
            pltpu.make_async_remote_copy(
                src_ref=src_of(to), dst_ref=dst,
                send_sem=send_sem.at[i], recv_sem=recv_sem.at[i],
                device_id={"tp": to}, device_id_type=MESH,
            ).start()

    all_of(0, tok_out, tok_in).wait_recv()
    wide[...] = tok_in[...].reshape(slots * 4, 128).astype(F32)
    for b in range(4):
        rows_all[j, :, b * 128 : (b + 1) * 128] = wide[pl.ds(b, slots, stride=4), :].astype(BF16)
    across(4, lambda to: rows_all.at[j], rows_all.at[j])

    all_of(1, down_out, down_in).wait_recv()
    across(5, lambda to: down_in.at[pl.ds(to * (n_fs // n_tp), n_fs // n_tp)], down_q.at[j])
    down_q[j] = down_in[pl.ds(j * (n_fs // n_tp), n_fs // n_tp)]

    all_of(4, rows_all, rows_all, n_tp - 1).wait_recv()
    all_of(2, gate_out, gate_in).wait_recv()
    depth = n_fs // n_tp

    def product(w):
        total = None
        for k in range(n_tp):
            block = w[k * depth : (k + 1) * depth].reshape(depth * 16, 128)
            term = jnp.dot(rows_all[k], block, preferred_element_type=F32)
            total = term if total is None else total + term
        return total

    gate_acc = product(gate_in)
    all_of(3, up_out, up_in).wait_recv()
    up_acc = product(up_in)
    hidden = (gate_acc / (1.0 + jnp.exp(-gate_acc)) * up_acc).astype(BF16)
    per = slots // PIECES
    for h in range(PIECES):
        hid_all[h, j] = hidden[h * per : (h + 1) * per]
        across(6 + h, lambda to: hid_all.at[h, j], hid_all.at[h, j])
    all_of(5, down_q, down_q, n_tp - 1).wait_recv()

    for h in range(PIECES):
        all_of(6 + h, hid_all.at[h], hid_all.at[h], n_tp - 1).wait_recv()
        total = None
        for k in range(n_tp):
            term = lax.dot_general(
                hid_all[h, k], down_q[k].reshape(depth * 16, 128), (((1,), (1,)), ((), ())),
                preferred_element_type=F32,
            )
            total = term if total is None else total + term
        for b in range(4):
            wide[pl.ds(h * per * 4 + b, per, stride=4), :] = total[:, b * 128 : (b + 1) * 128]
        part = pl.ds(h * n_fs // PIECES, n_fs // PIECES)
        ret_out[part] = (
            wide[h * per * 4 : (h + 1) * per * 4].astype(BF16).reshape(n_fs // PIECES, 8, 128)
        )
        rows = 8 // PIECES
        torus.row_by_row(h * rows, (h + 1) * rows, sender(10, ret_out, ret_in))
    ret_in[me] = ret_out[me]

    here = lax.broadcasted_iota(jnp.int32, (count, count), 0) == lax.broadcasted_iota(
        jnp.int32, (count, count), 1
    )
    w_first = group[...] * jax.nn.sigmoid(gap[...])
    w_second = group[...] * jax.nn.sigmoid(-gap[...])
    w_first = jnp.sum(jnp.where(here, w_first, 0.0), axis=1, keepdims=True)
    w_second = jnp.sum(jnp.where(here, w_second, 0.0), axis=1, keepdims=True)

    all_of(10, ret_out, ret_in).wait_recv()
    wide[...] = ret_in[...].reshape(slots * 4, 128).astype(F32)
    for b in range(4):
        block = wide[pl.ds(b, slots, stride=4), :].astype(BF16)
        value = [
            lax.dot_general(
                picks[k], block, (((0,), (0,)), ((), ())), preferred_element_type=F32
            )
            for k in range(2)
        ]
        mixed_ref[:, b * 128 : (b + 1) * 128] = (
            w_first * value[0] + w_second * value[1]
        ).astype(BF16)

    for i, (src, dst) in enumerate(
        [(tok_out, tok_in), (down_out, down_in), (gate_out, gate_in), (up_out, up_in)]
    ):
        all_of(i, src, dst).wait_send()
    for i, a in [(4, rows_all), (5, down_q)] + [(6 + h, hid_all.at[h]) for h in range(PIECES)]:
        all_of(i, a, a, n_tp - 1).wait_send()
    all_of(10, ret_out, ret_in).wait_send()


def place(gate_in, up_in, down_in, mixed_in, gate_ref, up_ref, down_ref, mixed_ref, sem):
    copies = [
        pltpu.make_async_copy(src, dst, sem.at[i])
        for i, (src, dst) in enumerate(
            [(gate_in, gate_ref), (up_in, up_ref), (down_in, down_ref), (mixed_in, mixed_ref)]
        )
    ]
    for c in copies:
        c.start()
    for c in copies:
        c.wait()


def body(
    tokens, norm_gain, gate_weight, up_weight, down_weight, route_ids, group_weight, logit_gap
):
    n_fs, n_tp = lax.axis_size("fs"), lax.axis_size("tp")
    count, width = tokens.shape
    experts, depth, units = gate_weight.shape
    whole = pl.BlockSpec(memory_space=pltpu.VMEM)
    anywhere = pl.BlockSpec(memory_space=pltpu.HBM)
    weights = jax.ShapeDtypeStruct((experts, depth, units), BF16)
    slots = 2 * n_fs
    results = (weights, weights, weights, jax.ShapeDtypeStruct((count, width), BF16))
    held = pl.pallas_call(
        functools.partial(kernel, n_fs, n_tp),
        out_shape=tuple(pltpu.VMEM(r.shape, r.dtype) for r in results),
        in_specs=[anywhere] * 8,
        out_specs=[whole] * 4,
        scratch_shapes=[
            pltpu.VMEM((2, count), jnp.int32),
            pltpu.VMEM((1, count), F32),
            pltpu.VMEM((1, count), F32),
            pltpu.VMEM((1, depth), F32),
            pltpu.VMEM((count, width), BF16),
        ]
        + [pltpu.VMEM((experts, depth, units), F32)] * 3
        + [pltpu.VMEM((experts, depth, units), BF16)] * 3
        + [pltpu.VMEM((n_fs, 8, 128), BF16)] * 4
        + [
            pltpu.VMEM((n_tp, slots, width), BF16),
            pltpu.VMEM((PIECES, n_tp, slots // PIECES, units), BF16),
            pltpu.VMEM((n_tp, n_fs // n_tp, depth, units), BF16),
            pltpu.VMEM((slots * 4, 128), F32),
            pltpu.VMEM((2, slots, count), BF16),
            pltpu.SemaphoreType.DMA((8,)),
            pltpu.SemaphoreType.DMA((7 + PIECES,)),
            pltpu.SemaphoreType.DMA((7 + PIECES,)),
        ],
        compiler_params=pltpu.CompilerParams(
            collective_id=0, has_side_effects=True, vmem_limit_bytes=65404928 - 8192
        ),
    )(
        route_ids.T, group_weight.reshape(1, count), logit_gap.reshape(1, count),
        norm_gain.reshape(1, depth), tokens, gate_weight, up_weight, down_weight,
    )
    gate_new, up_new, down_new, mixed = pl.pallas_call(
        place,
        out_shape=results,
        in_specs=[whole] * 4,
        out_specs=[anywhere] * 4,
        scratch_shapes=[pltpu.SemaphoreType.DMA((4,))],
        compiler_params=pltpu.CompilerParams(vmem_limit_bytes=4 * 1024 * 1024),
    )(*held)
    shape = (1, experts * depth, units)
    return gate_new.reshape(shape), up_new.reshape(shape), down_new.reshape(shape), mixed


def solution(mesh):
    return jax.shard_map(
        body,
        mesh=mesh,
        in_specs=(
            P("fs", "tp"), P("fs"), P(None, "fs", "tp"), P(None, "fs", "tp"),
            P(None, "fs", "tp"), P("fs", None), P("fs"), P("fs"),
        ),
        out_specs=(P("fs", None, "tp"), P("fs", None, "tp"), P("fs", None, "tp"), P("fs", "tp")),
        check_vma=False,
    )
```

```python
import functools

import jax
import jax.numpy as jnp
from jax import lax
from jax.experimental import pallas as pl
from jax.experimental.pallas import tpu as pltpu
from jax.sharding import PartitionSpec as P

MESH = pl.DeviceIdType.MESH
F32, BF16 = jnp.float32, jnp.bfloat16
FAR_FIRST = (4, 3, 5, 2, 6, 1, 7, 0)
NEARING = sorted(
    ((a, b) for a in range(8) for b in range(8)),
    key=lambda t: -sum(min(FAR_FIRST[i], 8 - FAR_FIRST[i]) for i in t),
)
PIECES = 4


class Torus:
    def __init__(self, me):
        self.z, y, self.c = me // 16, (me // 2) % 8, me % 2
        self.places = [((y + dy) % 8) * 2 for dy in FAR_FIRST]
        self.columns = [at + (self.c + dc) % 2 for at in self.places for dc in (1, 0)]
        self.rows = tuple(((self.z + dz) % 8) * 16 for dz in FAR_FIRST)

    def far_first(self, step):
        def turn(_, rows):
            for column in self.columns:
                step(rows[0] + column)
            return rows[1:] + rows[:1]

        rows = lax.fori_loop(0, 7, turn, self.rows)
        for column in self.columns[:-1]:
            step(rows[0] + column)

    def of_core_far_first(self, core, step):
        for a, b in NEARING:
            if a < 7 or b < 7:
                step(self.rows[a] + self.places[b] + core)

        @pl.when(self.c != core)
        def _():
            step(self.rows[7] + self.places[7] + core)

    def of_core(self, core, step):
        own, columns = self.c == core, [at + core for at in self.places]

        def turn(_, rows):
            for u, column in enumerate(columns):
                step(rows[(3 * u + 2) % 8] + column)
            return rows[1:] + rows[:1]

        for u, column in enumerate(columns[:-1]):
            step(self.rows[(3 * u + 2) % 8] + column)

        @pl.when(jnp.logical_not(own))
        def _():
            step(self.rows[-1] + columns[-1])

        lax.fori_loop(1, 8, turn, self.rows[1:] + self.rows[:1])

    def row_by_row(self, low, high, step):
        def turn(row, _):
            for column in self.columns[:-1]:
                step(row * 16 + column)

            @pl.when(row != self.z)
            def _():
                step(row * 16 + self.columns[-1])

            return 0

        lax.fori_loop(low, high, turn, 0)


def kernel(
    n_fs, n_tp,
    ids_ref, group_ref, gap_ref, gain_ref, tokens_ref, gate_ref, up_ref, down_ref,
    gate_in, up_in, down_in, ret_in, picks, shares,
    ids, group, gap, gain, tokens, gate_f, up_f, down_f,
    gate_out, up_out, down_out, tok_out, tok_in, ret_out,
    rows_all, hid_all, down_q, wide,
    local_sem, send_sem, recv_sem,
):
    me, j = lax.axis_index("fs"), lax.axis_index("tp")
    slots = 2 * n_fs
    torus = Torus(me)
    barrier = pltpu.get_barrier_semaphore()

    def greet(d):
        pl.semaphore_signal(barrier, inc=1, device_id={"fs": d}, device_id_type=MESH)

    small = [(ids_ref, ids), (group_ref, group), (gap_ref, gap), (gain_ref, gain), (tokens_ref, tokens)]
    large = [(down_ref, down_f), (gate_ref, gate_f), (up_ref, up_f)]
    loads = [
        pltpu.make_async_copy(src, dst, local_sem.at[i])
        for i, (src, dst) in enumerate(small + large)
    ]
    for c in loads:
        c.start()
    torus.far_first(greet)
    for k in range(1, n_tp):
        pl.semaphore_signal(
            barrier, inc=1, device_id={"tp": (j + k) % n_tp}, device_id_type=MESH
        )
    for c in loads[:5]:
        c.wait()

    count = tokens.shape[0]
    slot = lax.broadcasted_iota(jnp.int32, (slots, count), 0)
    first = (slot // 2 == ids[0:1, :]).astype(F32)
    second = (slot // 2 == ids[1:2, :]).astype(F32)
    earlier = (
        lax.broadcasted_iota(jnp.int32, (count, count), 0)
        < lax.broadcasted_iota(jnp.int32, (count, count), 1)
    ).astype(BF16)
    before = jnp.dot((first + second).astype(BF16), earlier, preferred_element_type=F32)
    ranked = (before == (slot % 2).astype(F32)).astype(F32)
    first, second = first * ranked, second * ranked
    picks[0] = first.astype(BF16)
    picks[1] = second.astype(BF16)
    outgoing = jnp.dot((first + second).astype(BF16), tokens[...], preferred_element_type=F32)
    for b in range(4):
        wide[pl.ds(b, slots, stride=4), :] = outgoing[:, b * 128 : (b + 1) * 128]
    tok_out[...] = wide[...].astype(BF16).reshape(n_fs, 8, 128)

    diagonal = lax.broadcasted_iota(jnp.int32, (16, 16), 0) == lax.broadcasted_iota(
        jnp.int32, (16, 16), 1
    )
    scale = jnp.sum(jnp.where(diagonal, gain[...], 0.0), axis=1, keepdims=True)
    scale = jnp.broadcast_to(scale, (16, 128))[None]

    def round_down(i, _):
        at = pl.ds(i * 8, 8)
        down_out[at] = down_f[at].astype(BF16)
        return 0

    def round_first(i, _):
        at = pl.ds(i * 8, 8)
        gate_out[at] = (gate_f[at] * scale).astype(BF16)
        up_out[at] = (up_f[at] * scale).astype(BF16)
        return 0

    pl.semaphore_wait(barrier, n_fs - 1 + n_tp - 1)

    def sender(i, src, dst):
        def send(d):
            pltpu.make_async_remote_copy(
                src_ref=src.at[d], dst_ref=dst.at[me],
                send_sem=send_sem.at[i], recv_sem=recv_sem.at[i],
                device_id={"fs": d}, device_id_type=MESH,
            ).start()

        return send

    def exchange(i, src, dst, core):
        torus.of_core(core, sender(i, src, dst))

    def all_of(i, src, dst, copies=n_fs - 1):
        return pltpu.make_async_remote_copy(
            src_ref=src.at[pl.ds(0, copies)], dst_ref=dst.at[pl.ds(0, copies)],
            send_sem=send_sem.at[i], recv_sem=recv_sem.at[i],
            device_id={"tp": (j + 1) % n_tp}, device_id_type=MESH,
        )

    exchange(0, tok_out, tok_in, 0)
    loads[5].wait()
    lax.fori_loop(0, n_fs // 8, round_down, 0)
    exchange(1, down_out, down_in, 0)
    loads[6].wait()
    loads[7].wait()
    lax.fori_loop(0, n_fs // 8, round_first, 0)
    exchange(2, gate_out, gate_in, 0)
    torus.of_core_far_first(0, sender(3, up_out, up_in))
    exchange(0, tok_out, tok_in, 1)
    exchange(1, down_out, down_in, 1)
    exchange(2, gate_out, gate_in, 1)
    torus.of_core_far_first(1, sender(3, up_out, up_in))
    for src, dst in ((tok_out, tok_in), (down_out, down_in), (gate_out, gate_in), (up_out, up_in)):
        dst[me] = src[me]

    def across(i, src_of, dst):
        for k in (2, 1, 3):
            to = (j + k) % n_tp
            pltpu.make_async_remote_copy(
                src_ref=src_of(to), dst_ref=dst,
                send_sem=send_sem.at[i], recv_sem=recv_sem.at[i],
                device_id={"tp": to}, device_id_type=MESH,
            ).start()

    all_of(0, tok_out, tok_in).wait_recv()
    wide[...] = tok_in[...].reshape(slots * 4, 128).astype(F32)
    for b in range(4):
        rows_all[j, :, b * 128 : (b + 1) * 128] = wide[pl.ds(b, slots, stride=4), :].astype(BF16)
    across(4, lambda to: rows_all.at[j], rows_all.at[j])

    all_of(1, down_out, down_in).wait_recv()
    across(5, lambda to: down_in.at[pl.ds(to * (n_fs // n_tp), n_fs // n_tp)], down_q.at[j])
    down_q[j] = down_in[pl.ds(j * (n_fs // n_tp), n_fs // n_tp)]

    all_of(4, rows_all, rows_all, n_tp - 1).wait_recv()
    all_of(2, gate_out, gate_in).wait_recv()
    depth = n_fs // n_tp

    def product(w):
        total = None
        for k in range(n_tp):
            block = w[k * depth : (k + 1) * depth].reshape(depth * 16, 128)
            term = jnp.dot(rows_all[k], block, preferred_element_type=F32)
            total = term if total is None else total + term
        return total

    gate_acc = product(gate_in)
    all_of(3, up_out, up_in).wait_recv()
    up_acc = product(up_in)
    hidden = (gate_acc / (1.0 + jnp.exp(-gate_acc)) * up_acc).astype(BF16)
    per = slots // PIECES
    for h in range(PIECES):
        hid_all[h, j] = hidden[h * per : (h + 1) * per]
        across(6 + h, lambda to: hid_all.at[h, j], hid_all.at[h, j])
    all_of(5, down_q, down_q, n_tp - 1).wait_recv()

    for h in range(PIECES):
        all_of(6 + h, hid_all.at[h], hid_all.at[h], n_tp - 1).wait_recv()
        total = None
        for k in range(n_tp):
            term = lax.dot_general(
                hid_all[h, k], down_q[k].reshape(depth * 16, 128), (((1,), (1,)), ((), ())),
                preferred_element_type=F32,
            )
            total = term if total is None else total + term
        for b in range(4):
            wide[pl.ds(h * per * 4 + b, per, stride=4), :] = total[:, b * 128 : (b + 1) * 128]
        part = pl.ds(h * n_fs // PIECES, n_fs // PIECES)
        ret_out[part] = (
            wide[h * per * 4 : (h + 1) * per * 4].astype(BF16).reshape(n_fs // PIECES, 8, 128)
        )
        rows = 8 // PIECES
        torus.row_by_row(h * rows, (h + 1) * rows, sender(10, ret_out, ret_in))
    ret_in[me] = ret_out[me]

    here = lax.broadcasted_iota(jnp.int32, (count, count), 0) == lax.broadcasted_iota(
        jnp.int32, (count, count), 1
    )
    w_first = group[...] * jax.nn.sigmoid(gap[...])
    w_second = group[...] * jax.nn.sigmoid(-gap[...])
    for k, w in enumerate((w_first, w_second)):
        w = jnp.sum(jnp.where(here, w, 0.0), axis=1, keepdims=True)
        shares[k] = jnp.broadcast_to(w, (count, 128))

    all_of(10, ret_out, ret_in).wait_recv()
    for i, (src, dst) in enumerate(
        [(tok_out, tok_in), (down_out, down_in), (gate_out, gate_in), (up_out, up_in)]
    ):
        all_of(i, src, dst).wait_send()
    for i, a in [(4, rows_all), (5, down_q)] + [(6 + h, hid_all.at[h]) for h in range(PIECES)]:
        all_of(i, a, a, n_tp - 1).wait_send()
    all_of(10, ret_out, ret_in).wait_send()


def finish(
    gate_in, up_in, down_in, ret_in, picks, shares,
    gate_ref, up_ref, down_ref, mixed_ref, wide, mixed, sem,
):
    pairs = [(gate_in, gate_ref), (up_in, up_ref), (down_in, down_ref), (mixed, mixed_ref)]
    copies = [pltpu.make_async_copy(src, dst, sem.at[i]) for i, (src, dst) in enumerate(pairs)]
    for c in copies[:3]:
        c.start()
    slots = picks.shape[1]
    wide[...] = ret_in[...].reshape(slots * 4, 128).astype(F32)
    for b in range(4):
        block = wide[pl.ds(b, slots, stride=4), :].astype(BF16)
        value = [
            lax.dot_general(
                picks[k], block, (((0,), (0,)), ((), ())), preferred_element_type=F32
            )
            for k in range(2)
        ]
        mixed[:, b * 128 : (b + 1) * 128] = (
            shares[0] * value[0] + shares[1] * value[1]
        ).astype(BF16)
    copies[3].start()
    for c in copies:
        c.wait()


def body(
    tokens, norm_gain, gate_weight, up_weight, down_weight, route_ids, group_weight, logit_gap
):
    n_fs, n_tp = lax.axis_size("fs"), lax.axis_size("tp")
    count, width = tokens.shape
    experts, depth, units = gate_weight.shape
    whole = pl.BlockSpec(memory_space=pltpu.VMEM)
    anywhere = pl.BlockSpec(memory_space=pltpu.HBM)
    weights = jax.ShapeDtypeStruct((experts, depth, units), BF16)
    slots = 2 * n_fs
    results = (weights, weights, weights, jax.ShapeDtypeStruct((count, width), BF16))
    held = pl.pallas_call(
        functools.partial(kernel, n_fs, n_tp),
        out_shape=(
            *(pltpu.VMEM(r.shape, r.dtype) for r in results[:3]),
            pltpu.VMEM((n_fs, 8, 128), BF16),
            pltpu.VMEM((2, slots, count), BF16),
            pltpu.VMEM((2, count, 128), F32),
        ),
        in_specs=[anywhere] * 8,
        out_specs=[whole] * 6,
        scratch_shapes=[
            pltpu.VMEM((2, count), jnp.int32),
            pltpu.VMEM((1, count), F32),
            pltpu.VMEM((1, count), F32),
            pltpu.VMEM((1, depth), F32),
            pltpu.VMEM((count, width), BF16),
        ]
        + [pltpu.VMEM((experts, depth, units), F32)] * 3
        + [pltpu.VMEM((experts, depth, units), BF16)] * 3
        + [pltpu.VMEM((n_fs, 8, 128), BF16)] * 3
        + [
            pltpu.VMEM((n_tp, slots, width), BF16),
            pltpu.VMEM((PIECES, n_tp, slots // PIECES, units), BF16),
            pltpu.VMEM((n_tp, n_fs // n_tp, depth, units), BF16),
            pltpu.VMEM((slots * 4, 128), F32),
            pltpu.SemaphoreType.DMA((8,)),
            pltpu.SemaphoreType.DMA((7 + PIECES,)),
            pltpu.SemaphoreType.DMA((7 + PIECES,)),
        ],
        compiler_params=pltpu.CompilerParams(
            collective_id=0, has_side_effects=True, vmem_limit_bytes=67043328 - 1572864 - 262144 - 131072 - 65536 - 8192
        ),
    )(
        route_ids.T, group_weight.reshape(1, count), logit_gap.reshape(1, count),
        norm_gain.reshape(1, depth), tokens, gate_weight, up_weight, down_weight,
    )
    gate_new, up_new, down_new, mixed = pl.pallas_call(
        finish,
        out_shape=results,
        in_specs=[whole] * 6,
        out_specs=[anywhere] * 4,
        scratch_shapes=[
            pltpu.VMEM((slots * 4, 128), F32),
            pltpu.VMEM((count, width), BF16),
            pltpu.SemaphoreType.DMA((4,)),
        ],
        compiler_params=pltpu.CompilerParams(vmem_limit_bytes=4 * 1024 * 1024),
    )(*held)
    shape = (1, experts * depth, units)
    return gate_new.reshape(shape), up_new.reshape(shape), down_new.reshape(shape), mixed


def solution(mesh):
    return jax.shard_map(
        body,
        mesh=mesh,
        in_specs=(
            P("fs", "tp"), P("fs"), P(None, "fs", "tp"), P(None, "fs", "tp"),
            P(None, "fs", "tp"), P("fs", None), P("fs"), P("fs"),
        ),
        out_specs=(P("fs", None, "tp"), P("fs", None, "tp"), P("fs", None, "tp"), P("fs", "tp")),
        check_vma=False,
    )
```
